32 devices in a mesh: grp: 2 (over y), sp: 4 (over z), tp: 4 (over x, core).
Axes of the slice: x: 2, y: 2, z: 4, core: 2. Of those that a mesh axis runs over, the one named last changes fastest.
Arguments:
- tokens: bfloat16 [1024, 2048], P(('grp', 'sp'), 'tp'), parts along dimension 0
- mix_gain: bfloat16 [2048], replicated, may hold values from 0.099609375 to 1.8984375
- w_conv_value: bfloat16 [2048, 1024], P('sp', 'tp'), may hold values from -0.125 to 0.125
- w_conv_outer: bfloat16 [2048, 1024], P('sp', 'tp'), may hold values from -0.125 to 0.125
- w_conv_inner: bfloat16 [2048, 1024], P('sp', 'tp'), may hold values from -0.125 to 0.125
- conv_kernel: bfloat16 [3, 1024], P(None, 'tp'), may hold values from -3.5 to 3.5
- w_q_down: bfloat16 [2048, 512], P(None, 'tp'), may hold values from -0.125 to 0.125
- w_kv_down: bfloat16 [2048, 256], P(None, 'tp'), may hold values from -0.125 to 0.125
- w_rope_key: bfloat16 [2048, 32], replicated, may hold values from -0.125 to 0.125
- q_gain: bfloat16 [512], replicated
- kv_gain: bfloat16 [256], replicated, may hold values from 0.099609375 to 1.8984375
- w_q_nope: bfloat16 [512, 1024], P(None, 'tp'), may hold values from -0.25 to 0.25
- w_q_rope: bfloat16 [512, 512], P(None, 'tp'), may hold values from -0.25 to 0.25
- w_k_nope: bfloat16 [256, 1024], P(None, 'tp'), may hold values from -0.375 to 0.375
- w_value: bfloat16 [256, 1024], P(None, 'tp'), may hold values from -0.375 to 0.375
- w_out_conv: bfloat16 [1024, 2048], P('tp'), may hold values from -0.1875 to 0.1875
- w_out_attn: bfloat16 [1024, 2048], P('tp'), may hold values from -1.5 to 1.5
Outputs:
- mixed: bfloat16 [1024, 2048], P(('grp', 'sp'), 'tp'), parts along dimension 0
The draws below stay inside these ranges and needn't reach their ends.
There are 2 independent parts, one for each index of `grp`. The reference program is written for one: setup_inputs(seed, part) draws one part's arguments, and reference() takes and returns one part's arrays. A program takes and returns all parts, laid end to end along the dimension named above; an argument that names none is the same for every part. Nothing has to cross between parts.
All inputs are finite; a program needn't handle non-finite values.
Results may differ from the reference program's by a relative error of at most 0.028.
Values may be sent and summed in bfloat16 or wider, within the bound.
No kernel may reach another device: no remote copies, remote signals or barrier semaphores. Data moves between devices by JAX's collectives and lax.ppermute only.
A program may use at most 64 MiB of HBM per device.

```python
import jax
import jax.numpy as jnp
from jax import lax

D = 2048
MLA_HEADS = 16
Q_LATENT = 512
KV_LATENT = 256
NOPE = 64
ROPE = 32
VALUE = 64
TAPS = 3
TOKENS = 512
CONV_WIDTH = 1024
N_TP = 4


def draw_tokens(key, part):
    first = jax.random.fold_in(key, 11)
    second = jax.random.fold_in(key, 12)
    column = jnp.arange(D, dtype=jnp.float32) / max(D - 1, 1)
    column_scale = jnp.exp(jnp.log(3.0) * column) * jnp.exp(jax.random.uniform(second, (D,), jnp.float32, -0.35, 0.35))
    base = jax.random.normal(first, (TOKENS, D), jnp.float32)
    return (base * column_scale[None, :]).astype(jnp.bfloat16)


def draw_q_gain(key, part):
    spread = jax.random.uniform(jax.random.fold_in(key, 21), (Q_LATENT,), jnp.float32, -1.0, 1.0)
    return (2.0 * (1.0 + 0.18 * spread)).astype(jnp.bfloat16)


def shard_levels(rng, extent, shards, low, high):
    def one(axis_at, parts):
        draws = jax.random.uniform(jax.random.fold_in(jax.random.fold_in(rng, 6), axis_at), (parts,), jnp.float32, low / len(shards), high / len(shards))
        return jnp.repeat(jnp.exp(draws), extent[axis_at] // parts).reshape((-1,) + (1,) * (len(extent) - axis_at - 1))

    loudness = one(*shards[0])
    for cut in shards[1:]:
        loudness = loudness * one(*cut)
    return loudness


def normal_values(own_key, shape, scale, bound, shards=(), held_as=jnp.bfloat16):
    drawn = jax.random.normal(own_key, shape, jnp.float32) * scale
    if len(shards) > 0:
        drawn = shard_levels(own_key, shape, shards, -0.22, 0.18) * drawn
    return jnp.clip(drawn, min=-bound, max=bound).astype(held_as)


def setup_inputs(seed: int = 0, part: int = 0) -> dict:
    keys = jax.random.split(jax.random.key(seed), 18)
    own_keys = jax.random.split(jax.random.fold_in(keys[17], part), 18)
    tokens = draw_tokens(jax.random.fold_in(jax.random.fold_in(keys[17], part), 71), part)
    mix_gain = jnp.clip(1.0 + 0.18 * jax.random.normal(keys[1], (D,), jnp.float32), 0.099609375, 1.8984375).astype(jnp.bfloat16)
    w_conv_value = normal_values(keys[2], (D, CONV_WIDTH), D ** -0.5, 0.125, ((0, 4), (1, 4)))
    w_conv_outer = normal_values(keys[3], (D, CONV_WIDTH), D ** -0.5, 0.125, ((0, 4), (1, 4)))
    w_conv_inner = normal_values(keys[4], (D, CONV_WIDTH), D ** -0.5, 0.125, ((0, 4), (1, 4)))
    conv_kernel = normal_values(keys[5], (TAPS, CONV_WIDTH), TAPS ** -0.5, 3.5, ((1, 4),))
    w_q_down = normal_values(keys[6], (D, Q_LATENT), D ** -0.5, 0.125, ((1, 4),))
    w_kv_down = normal_values(keys[7], (D, KV_LATENT), D ** -0.5, 0.125, ((1, 4),))
    w_rope_key = normal_values(keys[8], (D, ROPE), D ** -0.5, 0.125)
    q_gain = draw_q_gain(jax.random.fold_in(keys[17], 71), part)
    kv_gain = jnp.clip(1.0 + 0.18 * jax.random.normal(keys[10], (KV_LATENT,), jnp.float32), 0.099609375, 1.8984375).astype(jnp.bfloat16)
    w_q_nope = normal_values(keys[11], (Q_LATENT, MLA_HEADS * NOPE), Q_LATENT ** -0.5, 0.25, ((1, 4),))
    w_q_rope = normal_values(keys[12], (Q_LATENT, MLA_HEADS * ROPE), Q_LATENT ** -0.5, 0.25, ((1, 4),))
    w_k_nope = normal_values(keys[13], (KV_LATENT, MLA_HEADS * NOPE), KV_LATENT ** -0.5, 0.375, ((1, 4),))
    w_value = normal_values(keys[14], (KV_LATENT, MLA_HEADS * VALUE), KV_LATENT ** -0.5, 0.375, ((1, 4),))
    w_out_conv = normal_values(keys[15], (CONV_WIDTH, D), CONV_WIDTH ** -0.5, 0.1875, ((0, 4),))
    w_out_attn = normal_values(keys[16], (MLA_HEADS * VALUE, D), (max(1, MLA_HEADS * VALUE // 64)) ** -0.5, 1.5, ((0, 4),))
    return dict(tokens=tokens, mix_gain=mix_gain, w_conv_value=w_conv_value, w_conv_outer=w_conv_outer, w_conv_inner=w_conv_inner, conv_kernel=conv_kernel, w_q_down=w_q_down, w_kv_down=w_kv_down, w_rope_key=w_rope_key, q_gain=q_gain, kv_gain=kv_gain, w_q_nope=w_q_nope, w_q_rope=w_q_rope, w_k_nope=w_k_nope, w_value=w_value, w_out_conv=w_out_conv, w_out_attn=w_out_attn)


EPS = 1e-06
THETA = 10000.0

def rms_scale(values):
    return lax.rsqrt(lax.optimization_barrier(jnp.mean(values * values, axis=-1, keepdims=True)) + EPS)

def angles(positions, width):
    inverse = THETA ** (-jnp.arange(0, width, 2, dtype=jnp.float32) / width)
    phase = positions[:, None] * inverse[None, :]
    phase = jnp.concatenate([phase, phase], axis=-1)
    return (jnp.cos(phase), jnp.sin(phase))

def turned(values, cosine, sine):
    half = values.shape[-1] // 2
    first = values[..., :half]
    second = values[..., half:]
    return values * cosine + jnp.concatenate([-second, first], axis=-1) * sine

def reference(tokens, mix_gain, w_conv_value, w_conv_outer, w_conv_inner, conv_kernel, w_q_down, w_kv_down, w_rope_key, q_gain, kv_gain, w_q_nope, w_q_rope, w_k_nope, w_value, w_out_conv, w_out_attn):
    f32 = jnp.float32
    bf16 = jnp.bfloat16
    inputs = tokens.astype(f32)
    row_scale = rms_scale(inputs)
    scaled = (inputs * mix_gain.astype(f32)).astype(bf16)

    def project(weight):
        return (row_scale * jnp.dot(scaled, weight, preferred_element_type=f32)).astype(bf16)
    conv_value = project(w_conv_value)
    conv_outer = project(w_conv_outer)
    conv_inner = project(w_conv_inner)
    q_latent = project(w_q_down)
    kv_latent = project(w_kv_down)
    rope_raw = project(w_rope_key)
    gated = (conv_inner.astype(f32) * conv_value.astype(f32)).astype(bf16)
    padded = jnp.pad(gated.astype(f32), ((1, 1), (0, 0)))
    kernel = conv_kernel.astype(f32)
    conv_out = padded[:-2] * kernel[0] + padded[1:-1] * kernel[1] + padded[2:] * kernel[2]
    y_conv = (conv_outer.astype(f32) * conv_out).astype(bf16)
    q_float = q_latent.astype(f32)
    q_normed = (q_float * rms_scale(q_float) * q_gain.astype(f32)).astype(bf16)
    kv_float = kv_latent.astype(f32)
    kv_normed = (kv_float * rms_scale(kv_float) * kv_gain.astype(f32)).astype(bf16)
    count = tokens.shape[0]
    heads = w_q_nope.shape[1] // NOPE
    positions = jnp.arange(count, dtype=f32)
    cosine, sine = angles(positions, ROPE)
    q_nope = jnp.dot(q_normed, w_q_nope, preferred_element_type=f32).astype(bf16).reshape(count, heads, NOPE)
    q_rope_raw = jnp.dot(q_normed, w_q_rope, preferred_element_type=f32).reshape(count, heads, ROPE)
    q_rope = turned(q_rope_raw, cosine[:, None, :], sine[:, None, :]).astype(bf16)
    k_nope = jnp.dot(kv_normed, w_k_nope, preferred_element_type=f32).astype(bf16).reshape(count, heads, NOPE)
    values = jnp.dot(kv_normed, w_value, preferred_element_type=f32).astype(bf16).reshape(count, heads, VALUE)
    k_rope = turned(rope_raw.astype(f32), cosine, sine).astype(bf16)
    factor = (NOPE + ROPE) ** (-0.5)
    block = 128 if count % 128 == 0 else count
    keys_f = k_nope.astype(f32)
    rope_f = k_rope.astype(f32)
    values_f = values.astype(f32)

    def attend(pieces):
        query_nope, query_rope = pieces
        scores = jnp.einsum('qhd,khd->qhk', query_nope.astype(f32), keys_f)
        scores = scores + jnp.einsum('qhr,kr->qhk', query_rope.astype(f32), rope_f)
        scores = scores * factor
        peak = lax.optimization_barrier(jnp.max(scores, axis=-1, keepdims=True))
        weights = jnp.exp(scores - peak)
        total = lax.optimization_barrier(jnp.sum(weights, axis=-1))
        summed = jnp.einsum('qhk,khd->qhd', weights.astype(bf16).astype(f32), values_f)
        return (summed / total[..., None]).astype(bf16)
    blocks = count // block
    result = lax.map(attend, (q_nope.reshape(blocks, block, heads, NOPE), q_rope.reshape(blocks, block, heads, ROPE)))
    y_attn = result.reshape(count, heads * VALUE)
    conv_share = y_conv.shape[1] // N_TP
    attn_share = y_attn.shape[1] // N_TP
    summed = jnp.zeros((count, w_out_conv.shape[1]), f32)
    for index in range(N_TP):
        conv_rows = slice(index * conv_share, (index + 1) * conv_share)
        attn_rows = slice(index * attn_share, (index + 1) * attn_share)
        partial_sum = jnp.dot(y_conv[:, conv_rows], w_out_conv[conv_rows], preferred_element_type=f32)
        partial_sum = partial_sum + jnp.dot(y_attn[:, attn_rows], w_out_attn[attn_rows], preferred_element_type=f32)
        summed = summed + lax.optimization_barrier(partial_sum.astype(bf16)).astype(f32)
    return summed.astype(bf16)
```

```python
import jax
import jax.numpy as jnp
from jax import lax
from jax.sharding import PartitionSpec as P

NOPE = 64
ROPE = 32
VALUE = 64


EPS = 1e-06
THETA = 10000.0

DIRECT = 8


def rms_scale(values):
    return lax.rsqrt(jnp.mean(values * values, axis=-1, keepdims=True) + EPS)


def angles(positions, width):
    inverse = THETA ** (-jnp.arange(0, width, 2, dtype=jnp.float32) / width)
    phase = positions[:, None] * inverse[None, :]
    phase = jnp.concatenate([phase, phase], axis=-1)
    return (jnp.cos(phase), jnp.sin(phase))


def turned(values, cosine, sine):
    half = values.shape[-1] // 2
    first = values[..., :half]
    second = values[..., half:]
    return values * cosine + jnp.concatenate([-second, first], axis=-1) * sine


def block_rows(count):
    for candidate in range(min(count, 1024), 0, -1):
        if count % candidate == 0 and candidate % 128 == 0:
            return candidate
    for candidate in range(min(count, 1024), 0, -1):
        if count % candidate == 0:
            return candidate
    return count


def shifted(x, axis, shift):
    size = lax.axis_size(axis)
    if shift % size == 0:
        return x
    return lax.ppermute(x, axis, [(i, (i + shift) % size) for i in range(size)])


def gathered_rows(x, axis):
    size = lax.axis_size(axis)
    if size > DIRECT:
        return lax.all_gather(x, axis, axis=0, tiled=True), False
    return jnp.concatenate([shifted(x, axis, j) for j in range(size)], axis=0), True


def span_blocks(x, axis, span):
    size = lax.axis_size(axis)
    if span > DIRECT:
        groups = [list(range(i, i + span)) for i in range(0, size, span)]
        return lax.all_gather(x, axis, axis_index_groups=groups)
    blocks = [x]
    for j in range(1, span):
        pairs = [(i, i // span * span + (i % span + j) % span) for i in range(size)]
        blocks.append(lax.ppermute(x, axis, pairs))
    return blocks


def per_device(
    tokens,
    mix_gain,
    w_conv_value,
    w_conv_outer,
    w_conv_inner,
    conv_kernel,
    w_q_down,
    w_kv_down,
    w_rope_key,
    q_gain,
    kv_gain,
    w_q_nope,
    w_q_rope,
    w_k_nope,
    w_value,
    w_out_conv,
    w_out_attn,
):
    f32 = jnp.float32
    bf16 = jnp.bfloat16
    rows = tokens.shape[0]
    size = lax.axis_size("sp")
    place = lax.axis_index("sp")
    n_tp = lax.axis_size("tp")
    place_tp = lax.axis_index("tp")
    span = size // 2 if size % 2 == 0 else size
    half = size // span - 1
    depth = w_conv_value.shape[0]

    def dot(a, b):
        return jnp.dot(a, b, preferred_element_type=f32)

    conv_ws = [span_blocks(w, "sp", span) for w in (w_conv_value, w_conv_outer, w_conv_inner)]
    base = place // span * span
    if span > DIRECT:
        owners = [base + j for j in range(span)]
    else:
        owners = [base + (place - base - j + span) % span for j in range(span)]

    piece = lax.all_gather(tokens, "tp", axis=1, tiled=True).astype(f32)
    normed = (piece * rms_scale(piece) * mix_gain.astype(f32)).astype(bf16)

    q_part = dot(normed, w_q_down).astype(bf16)
    kv_part = dot(normed, w_kv_down).astype(bf16)
    rope_raw = dot(normed, w_rope_key).astype(bf16)
    kv_width = kv_part.shape[1]
    packed, rotated = gathered_rows(jnp.concatenate([kv_part, rope_raw], axis=1), "sp")

    far = span * half
    if half:
        start = (place // span * -1 + 1) * span * depth
        for_partner = lax.dynamic_slice_in_dim(normed, start, span * depth, axis=1)
        theirs = shifted(for_partner, "sp", far)
        here = lax.dynamic_slice_in_dim(normed, base * depth, span * depth, axis=1)
        both = jnp.concatenate([theirs, here], axis=0)
    else:
        both = normed
    pieces = [
        lax.dynamic_slice_in_dim(both, (owner - base) * depth, depth, axis=1) for owner in owners
    ]
    sums = jnp.concatenate(
        [sum(dot(x, w) for x, w in zip(pieces, blocks)) for blocks in conv_ws], axis=1
    )
    width = w_conv_value.shape[1]
    if half:
        other = sums[:rows].astype(bf16)
        own = sums[rows:]
        edges = jnp.stack([own[0].astype(bf16), own[-1].astype(bf16), other[0], other[-1]])
        total = own + shifted(other, "sp", far).astype(f32)
    else:
        own = sums
        edges = jnp.stack([own[0].astype(bf16), own[-1].astype(bf16)])
        total = own
    moved = {}

    def edge_from(offset, index):
        key = -offset % size
        if key not in moved:
            moved[key] = shifted(edges, "sp", key).astype(f32)
        return moved[key][index : index + 1]

    before = edge_from(-1, 1)
    after = edge_from(1, 0)
    if half:
        before = before + edge_from(-1 + far, 3)
        after = after + edge_from(1 + far, 2)
    before = jnp.where(place > 0, before, 0.0)
    after = jnp.where(place < size - 1, after, 0.0)

    def gate(x):
        x = x.astype(bf16).astype(f32)
        return (x[:, 2 * width :] * x[:, :width]).astype(bf16).astype(f32)

    padded = jnp.concatenate([gate(before), gate(total), gate(after)], axis=0)
    kernel = conv_kernel.astype(f32)
    conv_out = padded[:-2] * kernel[0] + padded[1:-1] * kernel[1] + padded[2:] * kernel[2]
    y_conv = (total[:, width : 2 * width].astype(bf16).astype(f32) * conv_out).astype(bf16)

    q_float = lax.all_gather(q_part, "tp", axis=1, tiled=True).astype(f32)
    q_normed = (q_float * rms_scale(q_float) * q_gain.astype(f32)).astype(bf16)
    heads = w_q_nope.shape[1] // NOPE
    factor = (NOPE + ROPE) ** (-0.5)
    positions = (place * rows + jnp.arange(rows, dtype=jnp.int32)).astype(f32)
    cosine, sine = angles(positions, ROPE)
    q_nope = dot(q_normed, w_q_nope).astype(bf16).reshape(rows, heads, NOPE)
    q_rope_raw = dot(q_normed, w_q_rope).reshape(rows, heads, ROPE)
    q_rope = turned(q_rope_raw, cosine[:, None, :], sine[:, None, :]).astype(bf16)

    count = packed.shape[0]
    kv_all = lax.all_gather(packed[:, :kv_width], "tp", axis=1, tiled=True).astype(f32)
    latent = (kv_all * rms_scale(kv_all) * kv_gain.astype(f32)).astype(bf16)
    order = jnp.arange(count, dtype=jnp.int32)
    if rotated:
        order = (place - order // rows + size) % size * rows + order % rows
    key_cosine, key_sine = angles(order.astype(f32), ROPE)
    rope_keys = turned(packed[:, kv_width:].astype(f32), key_cosine, key_sine).astype(bf16)

    def scores_of(key_block, rope_block):
        keys3 = key_block.reshape(key_block.shape[0], heads, NOPE)
        scores = jnp.einsum("qhd,khd->hqk", q_nope, keys3, preferred_element_type=f32)
        scores = scores + jnp.einsum("qhr,kr->hqk", q_rope, rope_block, preferred_element_type=f32)
        return scores * factor

    def summed_of(weights, value_block):
        values3 = value_block.reshape(value_block.shape[0], heads, VALUE)
        return jnp.einsum("hqk,khd->hqd", weights.astype(bf16), values3, preferred_element_type=f32)

    step = block_rows(count)
    if step == count:
        scores = scores_of(dot(latent, w_k_nope).astype(bf16), rope_keys)
        weights = jnp.exp(scores - jnp.max(scores, axis=-1, keepdims=True))
        total_w = jnp.sum(weights, axis=-1)
        summed = summed_of(weights, dot(latent, w_value).astype(bf16))
    else:

        def one_block(state, blocks):
            peak, total_w, summed = state
            latent_block, rope_block = blocks
            scores = scores_of(dot(latent_block, w_k_nope).astype(bf16), rope_block)
            new_peak = jnp.maximum(peak, jnp.max(scores, axis=-1))
            fade = jnp.exp(peak - new_peak)
            weights = jnp.exp(scores - new_peak[..., None])
            total_w = total_w * fade + jnp.sum(weights, axis=-1)
            value_block = dot(latent_block, w_value).astype(bf16)
            summed = summed * fade[..., None] + summed_of(weights, value_block)
            return (new_peak, total_w, summed), None

        begin = (
            jnp.full((heads, rows), -jnp.inf, f32),
            jnp.zeros((heads, rows), f32),
            jnp.zeros((heads, rows, VALUE), f32),
        )
        (_, total_w, summed), _ = lax.scan(
            one_block,
            begin,
            (
                latent.reshape(count // step, step, latent.shape[1]),
                rope_keys.reshape(count // step, step, ROPE),
            ),
        )
    y_attn = (summed / total_w[..., None]).astype(bf16)
    y_attn = y_attn.transpose(1, 0, 2).reshape(rows, heads * VALUE)

    partial_sum = dot(y_conv, w_out_conv) + dot(y_attn, w_out_attn)
    columns = partial_sum.shape[1] // n_tp

    def share(target):
        return lax.dynamic_slice_in_dim(partial_sum, target * columns, columns, axis=1)

    result = share(place_tp)
    for k in range(1, n_tp):
        result = result + shifted(share((place_tp + k) % n_tp).astype(bf16), "tp", k).astype(f32)
    return result.astype(bf16)


def solution(mesh):
    placed = (
        P(("grp", "sp"), "tp"),
        P(),
        P("sp", "tp"),
        P("sp", "tp"),
        P("sp", "tp"),
        P(None, "tp"),
        P(None, "tp"),
        P(None, "tp"),
        P(),
        P(),
        P(),
        P(None, "tp"),
        P(None, "tp"),
        P(None, "tp"),
        P(None, "tp"),
        P("tp", None),
        P("tp", None),
    )
    return jax.shard_map(
        per_device, mesh=mesh, in_specs=placed, out_specs=P(("grp", "sp"), "tp"), check_vma=False
    )
```

```python
import functools

import jax
import jax.numpy as jnp
from jax import lax
from jax.experimental import pallas as pl
from jax.experimental.pallas import tpu as pltpu
from jax.sharding import PartitionSpec as P

NOPE = 64
ROPE = 32
VALUE = 64


EPS = 1e-06
THETA = 10000.0

DIRECT = 8


def rms_scale(values):
    return lax.rsqrt(jnp.mean(values * values, axis=-1, keepdims=True) + EPS)


def angles(positions, width):
    inverse = THETA ** (-jnp.arange(0, width, 2, dtype=jnp.float32) / width)
    phase = positions[:, None] * inverse[None, :]
    phase = jnp.concatenate([phase, phase], axis=-1)
    return (jnp.cos(phase), jnp.sin(phase))


def turned(values, cosine, sine):
    half = values.shape[-1] // 2
    first = values[..., :half]
    second = values[..., half:]
    return values * cosine + jnp.concatenate([-second, first], axis=-1) * sine


def block_rows(count):
    for candidate in range(min(count, 1024), 0, -1):
        if count % candidate == 0 and candidate % 128 == 0:
            return candidate
    for candidate in range(min(count, 1024), 0, -1):
        if count % candidate == 0:
            return candidate
    return count


def shifted(x, axis, shift):
    size = lax.axis_size(axis)
    if shift % size == 0:
        return x
    return lax.ppermute(x, axis, [(i, (i + shift) % size) for i in range(size)])


def gathered_rows(x, axis):
    size = lax.axis_size(axis)
    if size > DIRECT:
        return lax.all_gather(x, axis, axis=0, tiled=True), False
    return jnp.concatenate([shifted(x, axis, j) for j in range(size)], axis=0), True


def span_blocks(x, axis, span):
    size = lax.axis_size(axis)
    if span > DIRECT:
        groups = [list(range(i, i + span)) for i in range(0, size, span)]
        return lax.all_gather(x, axis, axis_index_groups=groups)
    blocks = [x]
    for j in range(1, span):
        pairs = [(i, i // span * span + (i % span + j) % span) for i in range(size)]
        blocks.append(lax.ppermute(x, axis, pairs))
    return blocks


def per_device_wide(
    tokens,
    mix_gain,
    w_conv_value,
    w_conv_outer,
    w_conv_inner,
    conv_kernel,
    w_q_down,
    w_kv_down,
    w_rope_key,
    q_gain,
    kv_gain,
    w_q_nope,
    w_q_rope,
    w_k_nope,
    w_value,
    w_out_conv,
    w_out_attn,
):
    f32 = jnp.float32
    bf16 = jnp.bfloat16
    rows = tokens.shape[0]
    size = lax.axis_size("sp")
    place = lax.axis_index("sp")
    n_tp = lax.axis_size("tp")
    place_tp = lax.axis_index("tp")
    span = size // 2 if size % 2 == 0 else size
    half = size // span - 1
    depth = w_conv_value.shape[0]

    def dot(a, b):
        return jnp.dot(a, b, preferred_element_type=f32)

    conv_ws = [span_blocks(w, "sp", span) for w in (w_conv_value, w_conv_outer, w_conv_inner)]
    base = place // span * span
    if span > DIRECT:
        owners = [base + j for j in range(span)]
    else:
        owners = [base + (place - base - j + span) % span for j in range(span)]

    piece = lax.all_gather(tokens, "tp", axis=1, tiled=True).astype(f32)
    normed = (piece * rms_scale(piece) * mix_gain.astype(f32)).astype(bf16)

    q_part = dot(normed, w_q_down).astype(bf16)
    kv_part = dot(normed, w_kv_down).astype(bf16)
    rope_raw = dot(normed, w_rope_key).astype(bf16)
    kv_width = kv_part.shape[1]
    packed, rotated = gathered_rows(jnp.concatenate([kv_part, rope_raw], axis=1), "sp")

    far = span * half
    if half:
        start = (place // span * -1 + 1) * span * depth
        for_partner = lax.dynamic_slice_in_dim(normed, start, span * depth, axis=1)
        theirs = shifted(for_partner, "sp", far)
        here = lax.dynamic_slice_in_dim(normed, base * depth, span * depth, axis=1)
        both = jnp.concatenate([theirs, here], axis=0)
    else:
        both = normed
    pieces = [
        lax.dynamic_slice_in_dim(both, (owner - base) * depth, depth, axis=1) for owner in owners
    ]
    sums = jnp.concatenate(
        [sum(dot(x, w) for x, w in zip(pieces, blocks)) for blocks in conv_ws], axis=1
    )
    width = w_conv_value.shape[1]
    if half:
        other = sums[:rows].astype(bf16)
        own = sums[rows:]
        edges = jnp.stack([own[0].astype(bf16), own[-1].astype(bf16), other[0], other[-1]])
        total = own + shifted(other, "sp", far).astype(f32)
    else:
        own = sums
        edges = jnp.stack([own[0].astype(bf16), own[-1].astype(bf16)])
        total = own
    moved = {}

    def edge_from(offset, index):
        key = -offset % size
        if key not in moved:
            moved[key] = shifted(edges, "sp", key).astype(f32)
        return moved[key][index : index + 1]

    before = edge_from(-1, 1)
    after = edge_from(1, 0)
    if half:
        before = before + edge_from(-1 + far, 3)
        after = after + edge_from(1 + far, 2)
    before = jnp.where(place > 0, before, 0.0)
    after = jnp.where(place < size - 1, after, 0.0)

    def gate(x):
        x = x.astype(bf16).astype(f32)
        return (x[:, 2 * width :] * x[:, :width]).astype(bf16).astype(f32)

    padded = jnp.concatenate([gate(before), gate(total), gate(after)], axis=0)
    kernel = conv_kernel.astype(f32)
    conv_out = padded[:-2] * kernel[0] + padded[1:-1] * kernel[1] + padded[2:] * kernel[2]
    y_conv = (total[:, width : 2 * width].astype(bf16).astype(f32) * conv_out).astype(bf16)

    q_float = lax.all_gather(q_part, "tp", axis=1, tiled=True).astype(f32)
    q_normed = (q_float * rms_scale(q_float) * q_gain.astype(f32)).astype(bf16)
    heads = w_q_nope.shape[1] // NOPE
    factor = (NOPE + ROPE) ** (-0.5)
    positions = (place * rows + jnp.arange(rows, dtype=jnp.int32)).astype(f32)
    cosine, sine = angles(positions, ROPE)
    q_nope = dot(q_normed, w_q_nope).astype(bf16).reshape(rows, heads, NOPE)
    q_rope_raw = dot(q_normed, w_q_rope).reshape(rows, heads, ROPE)
    q_rope = turned(q_rope_raw, cosine[:, None, :], sine[:, None, :]).astype(bf16)

    count = packed.shape[0]
    kv_all = lax.all_gather(packed[:, :kv_width], "tp", axis=1, tiled=True).astype(f32)
    latent = (kv_all * rms_scale(kv_all) * kv_gain.astype(f32)).astype(bf16)
    order = jnp.arange(count, dtype=jnp.int32)
    if rotated:
        order = (place - order // rows + size) % size * rows + order % rows
    key_cosine, key_sine = angles(order.astype(f32), ROPE)
    rope_keys = turned(packed[:, kv_width:].astype(f32), key_cosine, key_sine).astype(bf16)

    def scores_of(key_block, rope_block):
        keys3 = key_block.reshape(key_block.shape[0], heads, NOPE)
        scores = jnp.einsum("qhd,khd->hqk", q_nope, keys3, preferred_element_type=f32)
        scores = scores + jnp.einsum("qhr,kr->hqk", q_rope, rope_block, preferred_element_type=f32)
        return scores * factor

    def summed_of(weights, value_block):
        values3 = value_block.reshape(value_block.shape[0], heads, VALUE)
        return jnp.einsum("hqk,khd->hqd", weights.astype(bf16), values3, preferred_element_type=f32)

    step = block_rows(count)
    if step == count:
        scores = scores_of(dot(latent, w_k_nope).astype(bf16), rope_keys)
        weights = jnp.exp(scores - jnp.max(scores, axis=-1, keepdims=True))
        total_w = jnp.sum(weights, axis=-1)
        summed = summed_of(weights, dot(latent, w_value).astype(bf16))
    else:

        def one_block(state, blocks):
            peak, total_w, summed = state
            latent_block, rope_block = blocks
            scores = scores_of(dot(latent_block, w_k_nope).astype(bf16), rope_block)
            new_peak = jnp.maximum(peak, jnp.max(scores, axis=-1))
            fade = jnp.exp(peak - new_peak)
            weights = jnp.exp(scores - new_peak[..., None])
            total_w = total_w * fade + jnp.sum(weights, axis=-1)
            value_block = dot(latent_block, w_value).astype(bf16)
            summed = summed * fade[..., None] + summed_of(weights, value_block)
            return (new_peak, total_w, summed), None

        begin = (
            jnp.full((heads, rows), -jnp.inf, f32),
            jnp.zeros((heads, rows), f32),
            jnp.zeros((heads, rows, VALUE), f32),
        )
        (_, total_w, summed), _ = lax.scan(
            one_block,
            begin,
            (
                latent.reshape(count // step, step, latent.shape[1]),
                rope_keys.reshape(count // step, step, ROPE),
            ),
        )
    y_attn = (summed / total_w[..., None]).astype(bf16)
    y_attn = y_attn.transpose(1, 0, 2).reshape(rows, heads * VALUE)

    partial_sum = dot(y_conv, w_out_conv) + dot(y_attn, w_out_attn)
    columns = partial_sum.shape[1] // n_tp

    def share(target):
        return lax.dynamic_slice_in_dim(partial_sum, target * columns, columns, axis=1)

    result = share(place_tp)
    for k in range(1, n_tp):
        result = result + shifted(share((place_tp + k) % n_tp).astype(bf16), "tp", k).astype(f32)
    return result.astype(bf16)


f32 = jnp.float32
bf16 = jnp.bfloat16


def dot(a, b):
    return jnp.dot(a, b, preferred_element_type=f32)


def dot_t(a, b):
    return lax.dot_general(a, b, (((1,), (1,)), ((), ())), preferred_element_type=f32)


def swap(x, axis, code):
    size = lax.axis_size(axis)
    return lax.ppermute(x, axis, [(i, i ^ code) for i in range(size)])


def doubled(x, axis):
    size = lax.axis_size(axis)
    blocks, codes = [x], [0]
    bit = size // 2
    while bit:
        blocks = blocks + [swap(b, axis, bit) for b in blocks]
        codes = codes + [c ^ bit for c in codes]
        bit //= 2
    return blocks, codes


def call(kernel, outs, operands, scalars=1, name=None, flops=0):
    smem = pl.BlockSpec(memory_space=pltpu.SMEM)
    vmem = pl.BlockSpec(memory_space=pltpu.VMEM)
    moved = sum(o.size * o.dtype.itemsize for o in (*outs, *operands))
    return pl.pallas_call(
        kernel,
        out_shape=tuple(jax.ShapeDtypeStruct(o.shape, o.dtype) for o in outs),
        in_specs=[smem if i < scalars else vmem for i in range(len(operands))],
        out_specs=tuple(vmem for _ in outs),
        compiler_params=pltpu.CompilerParams(vmem_limit_bytes=24 * 2**20),
        cost_estimate=pl.CostEstimate(flops=flops, bytes_accessed=moved, transcendentals=0),
        name=name,
    )(*operands)


def like(shape, dtype):
    return jax.ShapeDtypeStruct(shape, dtype)


def rotated_lanes(x):
    width = x.shape[1]
    lane = lax.broadcasted_iota(jnp.int32, x.shape, 1)
    low = lane % ROPE < ROPE // 2
    return jnp.where(low, -pltpu.roll(x, width - ROPE // 2, 1), pltpu.roll(x, ROPE // 2, 1))


def down_kernel(parts, features, index, *refs):
    pieces = refs[:parts]
    gain, w_q, w_kv, w_rope, cosine, sine = refs[parts : parts + 6]
    near, far, q_out, kv_out, rope_out, normed = refs[parts + 6 :]
    width = pieces[0].shape[1]
    squares = sum(
        jnp.sum(p[...].astype(f32) * p[...].astype(f32), axis=1, keepdims=True) for p in pieces
    )
    scale = lax.rsqrt(squares / features + EPS)
    for j, piece in enumerate(pieces):
        at = pl.ds(pl.multiple_of(index[j] * width, width), width)
        normed[:, at] = (piece[...].astype(f32) * scale * gain[:, at].astype(f32)).astype(bf16)
    half = near.shape[1]
    near[...] = normed[:, pl.ds(pl.multiple_of(index[parts] * half, half), half)]
    far[...] = normed[:, pl.ds(pl.multiple_of(index[parts + 1] * half, half), half)]
    x = normed[...]
    q_out[...] = dot(x, w_q[...]).astype(bf16)
    kv = dot(x, w_kv[...])
    rows = kv.shape[0]
    packs = kv_out.shape[0]
    kv_out[...] = jnp.concatenate(
        [kv[i : i + packs] for i in range(0, rows, packs)], axis=1
    ).astype(bf16)
    rope = dot(x, w_rope[...]).astype(bf16).astype(f32)
    half_rope = rope.shape[1] // 2
    other = jnp.concatenate([-rope[:, half_rope:], rope[:, :half_rope]], axis=1)
    rope = rope * cosine[:, : rope.shape[1]] + other * sine[:, : rope.shape[1]]
    packs = rope_out.shape[0]
    rope_out[...] = jnp.concatenate(
        [rope[i : i + packs] for i in range(0, rows, packs)], axis=1
    ).astype(bf16)


def conv_kernel_of(blocks, mats, index, near, theirs, *refs):
    weights = refs[: blocks * mats]
    other_out, own_out, edge_out = refs[blocks * mats :]
    depth = weights[0].shape[0]
    width = weights[0].shape[1]
    edges = []
    for m in range(mats):
        other = own = None
        for b in range(blocks):
            at = pl.ds(pl.multiple_of(index[b] * depth, depth), depth)
            w = weights[m * blocks + b][...]
            o, h = dot(theirs[:, at], w), dot(near[:, at], w)
            other, own = (o, h) if other is None else (other + o, own + h)
        cols = slice(m * width, (m + 1) * width)
        other_out[:, cols] = other.astype(bf16)
        own_out[:, cols] = own
        edges.append(
            jnp.concatenate([own[:1], own[-1:], other[:1], other[-1:], own[:4]], axis=0)
        )
    edge_out[...] = jnp.concatenate(edges, axis=1).astype(bf16)


def attention_kernel(parts, packs, index, *refs):
    q_blocks = refs[:parts]
    kv_packs = refs[parts : parts + packs]
    q_gain, kv_gain, w_qn, w_qr, w_k, w_v, cosine, sine = refs[parts + packs : parts + packs + 8]
    y_out, q_all, lat, rope_all = refs[parts + packs + 8 :]
    rows = y_out.shape[0]
    heads = y_out.shape[1] // VALUE
    width = q_blocks[0].shape[1]
    for j, block in enumerate(q_blocks):
        q_all[:, pl.ds(pl.multiple_of(index[j] * width, width), width)] = block[:, :]
    q = q_all[...].astype(f32)
    q = q * lax.rsqrt(jnp.mean(q * q, axis=1, keepdims=True) + EPS)
    q = (q * q_gain[...].astype(f32)).astype(bf16)
    q_nope = dot(q, w_qn[...]).astype(bf16)
    q_rope = dot(q, w_qr[...])
    q_rope = (q_rope * cosine[...] + rotated_lanes(q_rope) * sine[...]).astype(bf16)
    part = w_k.shape[0] // parts
    lanes = kv_packs[0].shape[1]
    folds = lanes // part
    deep = rows // folds
    rope_folds = lanes // ROPE
    rope_deep = rows // rope_folds
    for i, pack in enumerate(kv_packs):
        for c in range(folds):
            lat[i * rows + c * deep : i * rows + (c + 1) * deep, :] = jnp.concatenate(
                [
                    pack[j * deep : (j + 1) * deep, c * part : (c + 1) * part].astype(f32)
                    for j in range(parts)
                ],
                axis=1,
            )
        begin = parts * deep
        for c in range(rope_folds):
            rope_all[i * rows + c * rope_deep : i * rows + (c + 1) * rope_deep, :] = pack[
                begin : begin + rope_deep, c * ROPE : (c + 1) * ROPE
            ]
    kv = lat[...]
    kv = kv * lax.rsqrt(jnp.mean(kv * kv, axis=1, keepdims=True) + EPS)
    kv = (kv * kv_gain[...].astype(f32)).astype(bf16)

    def rows_of(w):
        return jnp.concatenate(
            [w[pl.ds(pl.multiple_of(index[j] * part, part), part), :] for j in range(parts)],
            axis=0,
        )

    keys = dot(kv, rows_of(w_k)).astype(bf16)
    values = dot(kv, rows_of(w_v)).astype(bf16)
    factor = (NOPE + ROPE) ** (-0.5)
    rope_keys = rope_all[...]
    for h in range(heads):
        nope = slice(h * NOPE, (h + 1) * NOPE)
        scores = dot_t(q_nope[:, nope], keys[:, nope])
        scores = scores + dot_t(q_rope[:, h * ROPE : (h + 1) * ROPE], rope_keys)
        scores = scores * factor
        weights = jnp.exp(scores - jnp.max(scores, axis=1, keepdims=True))
        summed = dot(weights.astype(bf16), values[:, h * VALUE : (h + 1) * VALUE])
        y_out[:, h * VALUE : (h + 1) * VALUE] = (
            summed / jnp.sum(weights, axis=1, keepdims=True)
        ).astype(bf16)


def output_kernel(parts, far_edges, index, masks, own1, got1, own2, got2, *refs):
    from_before, from_after, mine = refs[:3]
    fars = refs[3 : 3 + far_edges]
    taps, y_attn, w_conv, w_attn = refs[3 + far_edges : 7 + far_edges]
    outs = refs[7 + far_edges :]
    width = w_conv.shape[0]

    def gate(x):
        x = x.astype(bf16).astype(f32)
        return (x[:, width:] * x[:, :width]).astype(bf16).astype(f32)

    def row(ref, at):
        return ref[...].astype(f32)[at : at + 1]

    before = masks[0] * row(from_before, 1) + masks[2] * row(mine, 3)
    after = masks[1] * row(from_after, 0) + masks[3] * row(mine, 2)
    before = before + masks[4] * row(fars[0], 3)
    after = after + masks[5] * row(fars[-1], 2)
    gated = gate(own1[...] + got1[...].astype(f32))
    rows = gated.shape[0]
    at = lax.broadcasted_iota(jnp.int32, gated.shape, 0)
    up = jnp.where(at == 0, gate(before), pltpu.roll(gated, 1, 0))
    down = jnp.where(at == rows - 1, gate(after), pltpu.roll(gated, rows - 1, 0))
    kernel = taps[...].astype(f32)
    conv_out = up * kernel[0:1] + gated * kernel[1:2] + down * kernel[2:3]
    outer = (own2[...] + got2[...].astype(f32)).astype(bf16).astype(f32)
    y_conv = (outer * conv_out).astype(bf16)
    columns = outs[0].shape[1]
    for k in range(parts):
        cols = pl.ds(pl.multiple_of(index[k] * columns, columns), columns)
        share = dot(y_conv, w_conv[:, cols]) + dot(y_attn[...], w_attn[:, cols])
        outs[k][...] = share.astype(outs[k].dtype)


def far_pairs(size):
    before = [(size - i, i) for i in range(1, size) if size - i != i]
    after = [(size - 2 - i, i) for i in range(size - 1) if size - 2 - i != i]
    return before, after


def per_device(
    tokens,
    mix_gain,
    w_conv_value,
    w_conv_outer,
    w_conv_inner,
    conv_kernel,
    w_q_down,
    w_kv_down,
    w_rope_key,
    q_gain,
    kv_gain,
    w_q_nope,
    w_q_rope,
    w_k_nope,
    w_value,
    w_out_conv,
    w_out_attn,
):
    rows = tokens.shape[0]
    size = lax.axis_size("sp")
    place = lax.axis_index("sp")
    n_tp = lax.axis_size("tp")
    place_tp = lax.axis_index("tp")
    span = size // 2
    features = tokens.shape[1] * n_tp
    width = w_conv_value.shape[1]
    half = place // span

    pieces, codes = doubled(tokens, "tp")
    tp_order = jnp.stack([place_tp ^ c for c in codes]).astype(jnp.int32)

    def span_of(w):
        return [w] + [swap(w, "sp", c) for c in range(1, span)]

    value_ws, inner_ws, outer_ws = span_of(w_conv_value), span_of(w_conv_inner), span_of(w_conv_outer)
    blocks = jnp.stack([place % span ^ c for c in range(span)]).astype(jnp.int32)

    positions = (place * rows + jnp.arange(rows, dtype=jnp.int32)).astype(f32)
    cosine, sine = angles(positions, ROPE)
    heads = w_q_nope.shape[1] // NOPE
    cosine, sine = jnp.tile(cosine, (1, heads)), jnp.tile(sine, (1, heads))

    kv_width = w_kv_down.shape[1]
    deep = rows * kv_width // 128
    rope_deep = rows * ROPE // 128
    near, far, q_part, kv_part, rope_part = pl.pallas_call(
        functools.partial(down_kernel, n_tp, features),
        out_shape=(
            like((rows, features // 2), bf16),
            like((rows, features // 2), bf16),
            like((rows, w_q_down.shape[1]), bf16),
            like((deep, 128), bf16),
            like((rope_deep, 128), bf16),
        ),
        in_specs=[pl.BlockSpec(memory_space=pltpu.SMEM)]
        + [pl.BlockSpec(memory_space=pltpu.VMEM)] * (n_tp + 6),
        out_specs=(pl.BlockSpec(memory_space=pltpu.VMEM),) * 5,
        scratch_shapes=[pltpu.VMEM((rows, features), bf16)],
        compiler_params=pltpu.CompilerParams(vmem_limit_bytes=24 * 2**20),
        cost_estimate=pl.CostEstimate(flops=10**8, bytes_accessed=3 * 10**6, transcendentals=0),
        name="down",
    )(
        jnp.concatenate([tp_order, jnp.stack([half, 1 - half]).astype(jnp.int32)]),
        *pieces,
        mix_gain[None],
        w_q_down,
        w_kv_down,
        w_rope_key,
        cosine,
        sine,
    )

    mirror = [(i, size - 1 - i) for i in range(size)]
    theirs = lax.ppermute(far, "sp", mirror)

    both, _ = doubled(jnp.concatenate([q_part, kv_part], axis=0), "tp")
    pack = jnp.concatenate([b[rows:] for b in both] + [rope_part], axis=0)
    packs = [pack] + [swap(pack, "sp", c) for c in range(1, size)]

    def partial_conv(groups, name):
        cols = width * len(groups)
        ws = [w for g in groups for w in g]
        return call(
            functools.partial(conv_kernel_of, span, len(groups)),
            (like((rows, cols), bf16), like((rows, cols), f32), like((8, cols), bf16)),
            (blocks, near, theirs, *ws),
            name=name,
            flops=4 * rows * features // 2 * cols,
        )

    other1, own1, edges = partial_conv((value_ws, inner_ws), "conv_gate")
    got1 = lax.ppermute(other1, "sp", mirror)
    from_before = lax.ppermute(edges, "sp", [(i, i + 1) for i in range(size - 1)])
    from_after = lax.ppermute(edges, "sp", [(i + 1, i) for i in range(size - 1)])
    pairs_before, pairs_after = far_pairs(size)
    if {a for a, _ in pairs_before} & {a for a, _ in pairs_after}:
        fars = [lax.ppermute(edges, "sp", p) for p in (pairs_before, pairs_after)]
    else:
        fars = [lax.ppermute(edges, "sp", pairs_before + pairs_after)]
    other2, own2, _ = partial_conv((outer_ws,), "conv_outer")
    got2 = lax.ppermute(other2, "sp", mirror)

    q_latent = n_tp * w_q_down.shape[1]
    kv_latent = n_tp * kv_width
    count = rows * size
    vmem = pl.BlockSpec(memory_space=pltpu.VMEM)
    y_attn = pl.pallas_call(
        functools.partial(attention_kernel, n_tp, size),
        out_shape=like((rows, heads * VALUE), bf16),
        in_specs=[pl.BlockSpec(memory_space=pltpu.SMEM)] + [vmem] * (n_tp + size + 8),
        out_specs=vmem,
        scratch_shapes=[
            pltpu.VMEM((rows, q_latent), bf16),
            pltpu.VMEM((count, kv_latent), f32),
            pltpu.VMEM((count, ROPE), bf16),
        ],
        compiler_params=pltpu.CompilerParams(vmem_limit_bytes=24 * 2**20),
        cost_estimate=pl.CostEstimate(flops=10**9, bytes_accessed=3 * 10**6, transcendentals=0),
        name="attention",
    )(
        tp_order,
        *[b[:rows] for b in both],
        *packs,
        q_gain[None],
        kv_gain.reshape(n_tp, kv_width)[tp_order].reshape(1, kv_latent),
        w_q_nope,
        w_q_rope,
        w_k_nope,
        w_value,
        cosine,
        sine,
    )

    last = size - 1
    self_before = place * 2 == size
    self_after = place * 2 == size - 2
    masks = jnp.stack(
        [
            place > 0,
            place < last,
            self_before,
            self_after,
            (place > 0) & ~self_before,
            (place < last) & ~self_after,
        ]
    ).astype(f32)
    columns = features // n_tp
    shares = call(
        functools.partial(output_kernel, n_tp, len(fars)),
        tuple(like((rows, columns), f32 if k == 0 else bf16) for k in range(n_tp)),
        (
            jnp.stack([place_tp ^ k for k in range(n_tp)]).astype(jnp.int32),
            masks,
            own1,
            got1,
            own2,
            got2,
            from_before,
            from_after,
            edges,
            *fars,
            conv_kernel,
            y_attn,
            w_out_conv,
            w_out_attn,
        ),
        scalars=2,
        name="output",
        flops=4 * rows * width * features,
    )
    result = shares[0]
    for k in range(n_tp - 1, 0, -1):
        result = result + swap(shares[k], "tp", k).astype(f32)
    return result.astype(bf16)


def solution(mesh):
    placed = (
        P(("grp", "sp"), "tp"),
        P(),
        P("sp", "tp"),
        P("sp", "tp"),
        P("sp", "tp"),
        P(None, "tp"),
        P(None, "tp"),
        P(None, "tp"),
        P(),
        P(),
        P(),
        P(None, "tp"),
        P(None, "tp"),
        P(None, "tp"),
        P(None, "tp"),
        P("tp", None),
        P("tp", None),
    )
    sp, tp = mesh.shape["sp"], mesh.shape["tp"]
    few = all(2 <= n <= DIRECT and n & (n - 1) == 0 for n in (sp, tp))
    return jax.shard_map(
        per_device if few else per_device_wide, mesh=mesh, in_specs=placed, out_specs=P(("grp", "sp"), "tp"), check_vma=False
    )
```

```python
import functools

import jax
import jax.numpy as jnp
from jax import lax
from jax.experimental import pallas as pl
from jax.experimental.pallas import tpu as pltpu
from jax.sharding import PartitionSpec as P

NOPE = 64
ROPE = 32
VALUE = 64


EPS = 1e-06
THETA = 10000.0

DIRECT = 8


def rms_scale(values):
    return lax.rsqrt(jnp.mean(values * values, axis=-1, keepdims=True) + EPS)


def angles(positions, width):
    inverse = THETA ** (-jnp.arange(0, width, 2, dtype=jnp.float32) / width)
    phase = positions[:, None] * inverse[None, :]
    phase = jnp.concatenate([phase, phase], axis=-1)
    return (jnp.cos(phase), jnp.sin(phase))


def turned(values, cosine, sine):
    half = values.shape[-1] // 2
    first = values[..., :half]
    second = values[..., half:]
    return values * cosine + jnp.concatenate([-second, first], axis=-1) * sine


def block_rows(count):
    for candidate in range(min(count, 1024), 0, -1):
        if count % candidate == 0 and candidate % 128 == 0:
            return candidate
    for candidate in range(min(count, 1024), 0, -1):
        if count % candidate == 0:
            return candidate
    return count


def shifted(x, axis, shift):
    size = lax.axis_size(axis)
    if shift % size == 0:
        return x
    return lax.ppermute(x, axis, [(i, (i + shift) % size) for i in range(size)])


def gathered_rows(x, axis):
    size = lax.axis_size(axis)
    if size > DIRECT:
        return lax.all_gather(x, axis, axis=0, tiled=True), False
    return jnp.concatenate([shifted(x, axis, j) for j in range(size)], axis=0), True


def span_blocks(x, axis, span):
    size = lax.axis_size(axis)
    if span > DIRECT:
        groups = [list(range(i, i + span)) for i in range(0, size, span)]
        return lax.all_gather(x, axis, axis_index_groups=groups)
    blocks = [x]
    for j in range(1, span):
        pairs = [(i, i // span * span + (i % span + j) % span) for i in range(size)]
        blocks.append(lax.ppermute(x, axis, pairs))
    return blocks


def per_device_wide(
    tokens,
    mix_gain,
    w_conv_value,
    w_conv_outer,
    w_conv_inner,
    conv_kernel,
    w_q_down,
    w_kv_down,
    w_rope_key,
    q_gain,
    kv_gain,
    w_q_nope,
    w_q_rope,
    w_k_nope,
    w_value,
    w_out_conv,
    w_out_attn,
):
    f32 = jnp.float32
    bf16 = jnp.bfloat16
    rows = tokens.shape[0]
    size = lax.axis_size("sp")
    place = lax.axis_index("sp")
    n_tp = lax.axis_size("tp")
    place_tp = lax.axis_index("tp")
    span = size // 2 if size % 2 == 0 else size
    half = size // span - 1
    depth = w_conv_value.shape[0]

    def dot(a, b):
        return jnp.dot(a, b, preferred_element_type=f32)

    conv_ws = [span_blocks(w, "sp", span) for w in (w_conv_value, w_conv_outer, w_conv_inner)]
    base = place // span * span
    if span > DIRECT:
        owners = [base + j for j in range(span)]
    else:
        owners = [base + (place - base - j + span) % span for j in range(span)]

    piece = lax.all_gather(tokens, "tp", axis=1, tiled=True).astype(f32)
    normed = (piece * rms_scale(piece) * mix_gain.astype(f32)).astype(bf16)

    q_part = dot(normed, w_q_down).astype(bf16)
    kv_part = dot(normed, w_kv_down).astype(bf16)
    rope_raw = dot(normed, w_rope_key).astype(bf16)
    kv_width = kv_part.shape[1]
    packed, rotated = gathered_rows(jnp.concatenate([kv_part, rope_raw], axis=1), "sp")

    far = span * half
    if half:
        start = (place // span * -1 + 1) * span * depth
        for_partner = lax.dynamic_slice_in_dim(normed, start, span * depth, axis=1)
        theirs = shifted(for_partner, "sp", far)
        here = lax.dynamic_slice_in_dim(normed, base * depth, span * depth, axis=1)
        both = jnp.concatenate([theirs, here], axis=0)
    else:
        both = normed
    pieces = [
        lax.dynamic_slice_in_dim(both, (owner - base) * depth, depth, axis=1) for owner in owners
    ]
    sums = jnp.concatenate(
        [sum(dot(x, w) for x, w in zip(pieces, blocks)) for blocks in conv_ws], axis=1
    )
    width = w_conv_value.shape[1]
    if half:
        other = sums[:rows].astype(bf16)
        own = sums[rows:]
        edges = jnp.stack([own[0].astype(bf16), own[-1].astype(bf16), other[0], other[-1]])
        total = own + shifted(other, "sp", far).astype(f32)
    else:
        own = sums
        edges = jnp.stack([own[0].astype(bf16), own[-1].astype(bf16)])
        total = own
    moved = {}

    def edge_from(offset, index):
        key = -offset % size
        if key not in moved:
            moved[key] = shifted(edges, "sp", key).astype(f32)
        return moved[key][index : index + 1]

    before = edge_from(-1, 1)
    after = edge_from(1, 0)
    if half:
        before = before + edge_from(-1 + far, 3)
        after = after + edge_from(1 + far, 2)
    before = jnp.where(place > 0, before, 0.0)
    after = jnp.where(place < size - 1, after, 0.0)

    def gate(x):
        x = x.astype(bf16).astype(f32)
        return (x[:, 2 * width :] * x[:, :width]).astype(bf16).astype(f32)

    padded = jnp.concatenate([gate(before), gate(total), gate(after)], axis=0)
    kernel = conv_kernel.astype(f32)
    conv_out = padded[:-2] * kernel[0] + padded[1:-1] * kernel[1] + padded[2:] * kernel[2]
    y_conv = (total[:, width : 2 * width].astype(bf16).astype(f32) * conv_out).astype(bf16)

    q_float = lax.all_gather(q_part, "tp", axis=1, tiled=True).astype(f32)
    q_normed = (q_float * rms_scale(q_float) * q_gain.astype(f32)).astype(bf16)
    heads = w_q_nope.shape[1] // NOPE
    factor = (NOPE + ROPE) ** (-0.5)
    positions = (place * rows + jnp.arange(rows, dtype=jnp.int32)).astype(f32)
    cosine, sine = angles(positions, ROPE)
    q_nope = dot(q_normed, w_q_nope).astype(bf16).reshape(rows, heads, NOPE)
    q_rope_raw = dot(q_normed, w_q_rope).reshape(rows, heads, ROPE)
    q_rope = turned(q_rope_raw, cosine[:, None, :], sine[:, None, :]).astype(bf16)

    count = packed.shape[0]
    kv_all = lax.all_gather(packed[:, :kv_width], "tp", axis=1, tiled=True).astype(f32)
    latent = (kv_all * rms_scale(kv_all) * kv_gain.astype(f32)).astype(bf16)
    order = jnp.arange(count, dtype=jnp.int32)
    if rotated:
        order = (place - order // rows + size) % size * rows + order % rows
    key_cosine, key_sine = angles(order.astype(f32), ROPE)
    rope_keys = turned(packed[:, kv_width:].astype(f32), key_cosine, key_sine).astype(bf16)

    def scores_of(key_block, rope_block):
        keys3 = key_block.reshape(key_block.shape[0], heads, NOPE)
        scores = jnp.einsum("qhd,khd->hqk", q_nope, keys3, preferred_element_type=f32)
        scores = scores + jnp.einsum("qhr,kr->hqk", q_rope, rope_block, preferred_element_type=f32)
        return scores * factor

    def summed_of(weights, value_block):
        values3 = value_block.reshape(value_block.shape[0], heads, VALUE)
        return jnp.einsum("hqk,khd->hqd", weights.astype(bf16), values3, preferred_element_type=f32)

    step = block_rows(count)
    if step == count:
        scores = scores_of(dot(latent, w_k_nope).astype(bf16), rope_keys)
        weights = jnp.exp(scores - jnp.max(scores, axis=-1, keepdims=True))
        total_w = jnp.sum(weights, axis=-1)
        summed = summed_of(weights, dot(latent, w_value).astype(bf16))
    else:

        def one_block(state, blocks):
            peak, total_w, summed = state
            latent_block, rope_block = blocks
            scores = scores_of(dot(latent_block, w_k_nope).astype(bf16), rope_block)
            new_peak = jnp.maximum(peak, jnp.max(scores, axis=-1))
            fade = jnp.exp(peak - new_peak)
            weights = jnp.exp(scores - new_peak[..., None])
            total_w = total_w * fade + jnp.sum(weights, axis=-1)
            value_block = dot(latent_block, w_value).astype(bf16)
            summed = summed * fade[..., None] + summed_of(weights, value_block)
            return (new_peak, total_w, summed), None

        begin = (
            jnp.full((heads, rows), -jnp.inf, f32),
            jnp.zeros((heads, rows), f32),
            jnp.zeros((heads, rows, VALUE), f32),
        )
        (_, total_w, summed), _ = lax.scan(
            one_block,
            begin,
            (
                latent.reshape(count // step, step, latent.shape[1]),
                rope_keys.reshape(count // step, step, ROPE),
            ),
        )
    y_attn = (summed / total_w[..., None]).astype(bf16)
    y_attn = y_attn.transpose(1, 0, 2).reshape(rows, heads * VALUE)

    partial_sum = dot(y_conv, w_out_conv) + dot(y_attn, w_out_attn)
    columns = partial_sum.shape[1] // n_tp

    def share(target):
        return lax.dynamic_slice_in_dim(partial_sum, target * columns, columns, axis=1)

    result = share(place_tp)
    for k in range(1, n_tp):
        result = result + shifted(share((place_tp + k) % n_tp).astype(bf16), "tp", k).astype(f32)
    return result.astype(bf16)


f32 = jnp.float32
bf16 = jnp.bfloat16


def dot(a, b):
    return jnp.dot(a, b, preferred_element_type=f32)


def dot_t(a, b):
    return lax.dot_general(a, b, (((1,), (1,)), ((), ())), preferred_element_type=f32)


def swap(x, axis, code):
    size = lax.axis_size(axis)
    return lax.ppermute(x, axis, [(i, i ^ code) for i in range(size)])


def doubled(x, axis):
    size = lax.axis_size(axis)
    blocks, codes = [x], [0]
    bit = size // 2
    while bit:
        blocks = blocks + [swap(b, axis, bit) for b in blocks]
        codes = codes + [c ^ bit for c in codes]
        bit //= 2
    return blocks, codes


def call(kernel, outs, operands, scalars=1, name=None, flops=0, scratch=()):
    smem = pl.BlockSpec(memory_space=pltpu.SMEM)
    vmem = pl.BlockSpec(memory_space=pltpu.VMEM)
    moved = sum(o.size * o.dtype.itemsize for o in (*outs, *operands))
    return pl.pallas_call(
        kernel,
        out_shape=tuple(jax.ShapeDtypeStruct(o.shape, o.dtype) for o in outs),
        in_specs=[smem if i < scalars else vmem for i in range(len(operands))],
        out_specs=tuple(vmem for _ in outs),
        scratch_shapes=list(scratch),
        compiler_params=pltpu.CompilerParams(vmem_limit_bytes=24 * 2**20),
        cost_estimate=pl.CostEstimate(flops=flops, bytes_accessed=moved, transcendentals=0),
        name=name,
    )(*operands)


def like(shape, dtype):
    return jax.ShapeDtypeStruct(shape, dtype)


def rotated_lanes(x):
    width = x.shape[1]
    lane = lax.broadcasted_iota(jnp.int32, x.shape, 1)
    low = lane % ROPE < ROPE // 2
    return jnp.where(low, -pltpu.roll(x, width - ROPE // 2, 1), pltpu.roll(x, ROPE // 2, 1))


def norm_kernel(parts, features, index, *refs):
    pieces, gain, normed, far = refs[:parts], *refs[parts:]
    width = pieces[0].shape[1]
    squares = sum(
        jnp.sum(p[...].astype(f32) * p[...].astype(f32), axis=1, keepdims=True) for p in pieces
    )
    scale = lax.rsqrt(squares / features + EPS)
    for j, piece in enumerate(pieces):
        at = pl.ds(pl.multiple_of(index[j] * width, width), width)
        normed[:, at] = (piece[...].astype(f32) * scale * gain[:, at].astype(f32)).astype(bf16)
    width = far.shape[1]
    far[...] = normed[:, pl.ds(pl.multiple_of(index[parts] * width, width), width)]


def down_kernel(x_ref, w_q, w_kv, w_rope, cosine, sine, q_out, keys_out):
    x = x_ref[...]
    kv = dot_t(x, w_kv[...])
    rows, width = kv.shape
    lanes = keys_out.shape[1]
    rope = dot_t(x, w_rope[...]).astype(bf16).astype(f32)
    half = ROPE // 2
    other = jnp.concatenate([-rope[:, half:], rope[:, :half]], axis=1)
    rope = rope * cosine[:, :ROPE] + other * sine[:, :ROPE]
    begin = 0
    for part in (kv, rope):
        deep = rows * part.shape[1] // lanes
        keys_out[begin : begin + deep, :] = jnp.concatenate(
            [part[i : i + deep] for i in range(0, rows, deep)], axis=1
        ).astype(bf16)
        begin += deep
    q_out[...] = dot(x, w_q[...]).astype(bf16)


def conv_kernel_of(blocks, mats, index, normed, first, second, *refs):
    weights = refs[: blocks * mats]
    other_out, own_out, edge_out, theirs = refs[blocks * mats :]
    depth, width = weights[0].shape
    piece = first.shape[1]
    for j, ref in enumerate((first, second)):
        theirs[:, pl.ds(pl.multiple_of(index[blocks + j] * piece, piece), piece)] = ref[...]
    base = index[blocks + 2] * (blocks * depth)
    edges = []
    for m in range(mats):
        other = own = None
        for b in range(blocks):
            at = pl.multiple_of(index[b] * depth, depth)
            w = weights[m * blocks + b][...]
            o = dot(theirs[:, pl.ds(at, depth)], w)
            h = dot(normed[:, pl.ds(pl.multiple_of(base + at, depth), depth)], w)
            other, own = (o, h) if other is None else (other + o, own + h)
        cols = slice(m * width, (m + 1) * width)
        other_out[:, cols] = other.astype(bf16)
        own_out[:, cols] = own
        edges.append(jnp.concatenate([own[:1], own[-1:], other[:1], other[-1:]] * 2, axis=0))
    edge_out[...] = jnp.concatenate(edges, axis=1).astype(bf16)


def attention_kernel(parts, packs, index, *refs):
    blocks = refs[:parts]
    ropes, q_gain, kv_gain, w_qn, w_qr, w_k, w_v, cosine, sine = refs[parts : parts + 9]
    y_out, q_all, lat, rope_all = refs[parts + 9 :]
    rows = y_out.shape[0]
    heads = y_out.shape[1] // VALUE
    width = blocks[0].shape[1]
    for j, block in enumerate(blocks):
        q_all[:, pl.ds(pl.multiple_of(index[j] * width, width), width)] = block[:rows, :]
    q = q_all[...].astype(f32)
    q = q * lax.rsqrt(jnp.mean(q * q, axis=1, keepdims=True) + EPS)
    q = (q * q_gain[...].astype(f32)).astype(bf16)
    q_nope = dot(q, w_qn[...]).astype(bf16)
    q_rope = dot(q, w_qr[...])
    q_rope = (q_rope * cosine[...] + rotated_lanes(q_rope) * sine[...]).astype(bf16)
    part = w_k.shape[0] // parts
    lanes = blocks[0].shape[1]
    folds = lanes // part
    deep = rows // folds
    rope_folds = lanes // ROPE
    rope_deep = rows // rope_folds
    for i in range(packs):
        at = rows + i * deep
        for c in range(folds):
            lat[i * rows + c * deep : i * rows + (c + 1) * deep, :] = jnp.concatenate(
                [b[at : at + deep, c * part : (c + 1) * part].astype(f32) for b in blocks], axis=1
            )
        at = i * rope_deep
        for c in range(rope_folds):
            rope_all[i * rows + c * rope_deep : i * rows + (c + 1) * rope_deep, :] = ropes[
                at : at + rope_deep, c * ROPE : (c + 1) * ROPE
            ]
    kv = lat[...]
    kv = kv * lax.rsqrt(jnp.mean(kv * kv, axis=1, keepdims=True) + EPS)
    kv = (kv * kv_gain[...].astype(f32)).astype(bf16)

    def rows_of(w):
        return jnp.concatenate(
            [w[pl.ds(pl.multiple_of(index[j] * part, part), part), :] for j in range(parts)],
            axis=0,
        )

    keys = dot(kv, rows_of(w_k)).astype(bf16)
    values = dot(kv, rows_of(w_v)).astype(bf16)
    factor = (NOPE + ROPE) ** (-0.5)
    rope_keys = rope_all[...]
    for h in range(heads):
        nope = slice(h * NOPE, (h + 1) * NOPE)
        scores = dot_t(q_nope[:, nope], keys[:, nope])
        scores = scores + dot_t(q_rope[:, h * ROPE : (h + 1) * ROPE], rope_keys)
        scores = scores * factor
        weights = jnp.exp(scores - jnp.max(scores, axis=1, keepdims=True))
        summed = dot(weights.astype(bf16), values[:, h * VALUE : (h + 1) * VALUE])
        y_out[:, h * VALUE : (h + 1) * VALUE] = (
            summed / jnp.sum(weights, axis=1, keepdims=True)
        ).astype(bf16)


def output_kernel(parts, sources, index, masks, own1, got1, own2, got2, *refs):
    edges = refs[:sources]
    taps, y_attn, w_conv, w_attn = refs[sources : 4 + sources]
    outs = refs[4 + sources :]
    width = w_conv.shape[0]

    def gate(x):
        x = x.astype(bf16).astype(f32)
        return (x[:, width:] * x[:, :width]).astype(bf16).astype(f32)

    before = after = 0.0
    for j, ref in enumerate(edges):
        e = ref[...].astype(f32)
        before = before + masks[4 * j + 1] * e[1:2] + masks[4 * j + 3] * e[3:4]
        after = after + masks[4 * j] * e[0:1] + masks[4 * j + 2] * e[2:3]
    gated = gate(own1[...] + got1[...].astype(f32))
    rows = gated.shape[0]
    at = lax.broadcasted_iota(jnp.int32, gated.shape, 0)
    up = jnp.where(at == 0, gate(before), pltpu.roll(gated, 1, 0))
    down = jnp.where(at == rows - 1, gate(after), pltpu.roll(gated, rows - 1, 0))
    kernel = taps[...].astype(f32)
    conv_out = up * kernel[0:1] + gated * kernel[1:2] + down * kernel[2:3]
    outer = (own2[...] + got2[...].astype(f32)).astype(bf16).astype(f32)
    y_conv = (outer * conv_out).astype(bf16)
    columns = outs[0].shape[1]
    for k in range(parts):
        cols = pl.ds(pl.multiple_of(index[k] * columns, columns), columns)
        share = dot(y_conv, w_conv[:, cols]) + dot(y_attn[...], w_attn[:, cols])
        outs[k][...] = share.astype(outs[k].dtype)


def edge_sources(size):
    half = size // 2
    table = {}
    for i in range(size):
        for step, own, far in ((-1, 1, 3), (1, 0, 2)):
            if 0 <= i + step < size:
                for source, edge in ((i + step, own), ((i + step) ^ half, far)):
                    table.setdefault(source ^ i, [[0.0] * 4 for _ in range(size)])[i][edge] = 1.0
    codes = sorted(table)
    return codes, [[v for c in codes for v in table[c][i]] for i in range(size)]


def per_device(
    tokens,
    mix_gain,
    w_conv_value,
    w_conv_outer,
    w_conv_inner,
    conv_kernel,
    w_q_down,
    w_kv_down,
    w_rope_key,
    q_gain,
    kv_gain,
    w_q_nope,
    w_q_rope,
    w_k_nope,
    w_value,
    w_out_conv,
    w_out_attn,
):
    rows = tokens.shape[0]
    size = lax.axis_size("sp")
    place = lax.axis_index("sp")
    n_tp = lax.axis_size("tp")
    place_tp = lax.axis_index("tp")
    span = size // 2
    features = tokens.shape[1] * n_tp
    width = w_conv_value.shape[1]
    half = place // span

    pieces, codes = doubled(tokens, "tp")
    tp_order = jnp.stack([place_tp ^ c for c in codes]).astype(jnp.int32)

    def span_of(w):
        return [w] + [swap(w, "sp", c) for c in range(1, span)]

    value_ws, inner_ws, outer_ws = span_of(w_conv_value), span_of(w_conv_inner), span_of(w_conv_outer)
    blocks = jnp.stack([place % span ^ c for c in range(span)]).astype(jnp.int32)

    positions = (place * rows + jnp.arange(rows, dtype=jnp.int32)).astype(f32)
    cosine, sine = angles(positions, ROPE)
    heads = w_q_nope.shape[1] // NOPE
    cosine, sine = jnp.tile(cosine, (1, heads)), jnp.tile(sine, (1, heads))

    kv_width = w_kv_down.shape[1]
    deep = rows * kv_width // 128
    rope_deep = rows * ROPE // 128
    core = place_tp % 2
    normed, far = call(
        functools.partial(norm_kernel, n_tp, features),
        (like((rows, features), bf16), like((rows, features // 4), bf16)),
        (
            jnp.concatenate([tp_order, (2 - 2 * half + core)[None].astype(jnp.int32)]),
            *pieces,
            mix_gain[None],
        ),
        name="norm",
        flops=10 * rows * features,
    )

    theirs = swap(far, "sp", span)
    theirs_too = swap(theirs, "tp", 1)

    q_part, keys = call(
        down_kernel,
        (like((rows, w_q_down.shape[1]), bf16), like((deep + rope_deep, 128), bf16)),
        (normed, w_q_down, w_kv_down.T, w_rope_key.T, cosine, sine),
        scalars=0,
        name="down",
        flops=2 * rows * features * (w_q_down.shape[1] + kv_width + ROPE),
    )
    packs = [keys]
    bit = 1
    while bit < size:
        packs = packs + [swap(p, "sp", bit) for p in [jnp.concatenate(packs, axis=0)]]
        bit *= 2
    packs = jnp.concatenate(packs, axis=0).reshape(size, deep + rope_deep, 128)
    ropes = packs[:, deep:].reshape(size * rope_deep, 128)
    both, _ = doubled(
        jnp.concatenate([q_part, packs[:, :deep].reshape(size * deep, 128)], axis=0), "tp"
    )
    conv_index = jnp.concatenate([blocks, jnp.stack([core, 1 - core, half]).astype(jnp.int32)])

    def partial_conv(groups, name):
        cols = width * len(groups)
        ws = [w for g in groups for w in g]
        return call(
            functools.partial(conv_kernel_of, span, len(groups)),
            (like((rows, cols), bf16), like((rows, cols), f32), like((8, cols), bf16)),
            (conv_index, normed, theirs, theirs_too, *ws),
            name=name,
            flops=4 * rows * features // 2 * cols,
            scratch=[pltpu.VMEM((rows, features // 2), bf16)],
        )

    other1, own1, edges = partial_conv((value_ws, inner_ws), "conv_gate")
    got1 = swap(other1, "sp", span)
    other2, own2, _ = partial_conv((outer_ws,), "conv_outer")
    got2 = swap(other2, "sp", span)
    edge_codes, edge_masks = edge_sources(size)
    edges = [swap(edges, "sp", c) if c else edges for c in edge_codes]

    q_latent = n_tp * w_q_down.shape[1]
    kv_latent = n_tp * kv_width
    count = rows * size
    vmem = pl.BlockSpec(memory_space=pltpu.VMEM)
    y_attn = pl.pallas_call(
        functools.partial(attention_kernel, n_tp, size),
        out_shape=like((rows, heads * VALUE), bf16),
        in_specs=[pl.BlockSpec(memory_space=pltpu.SMEM)] + [vmem] * (n_tp + 9),
        out_specs=vmem,
        scratch_shapes=[
            pltpu.VMEM((rows, q_latent), bf16),
            pltpu.VMEM((count, kv_latent), f32),
            pltpu.VMEM((count, ROPE), bf16),
        ],
        compiler_params=pltpu.CompilerParams(vmem_limit_bytes=24 * 2**20),
        cost_estimate=pl.CostEstimate(flops=10**9, bytes_accessed=3 * 10**6, transcendentals=0),
        name="attention",
    )(
        tp_order,
        *both,
        ropes,
        q_gain[None],
        kv_gain.reshape(n_tp, kv_width)[tp_order].reshape(1, kv_latent),
        w_q_nope,
        w_q_rope,
        w_k_nope,
        w_value,
        cosine,
        sine,
    )

    masks = jnp.asarray(edge_masks, f32)[place]
    columns = features // n_tp
    shares = call(
        functools.partial(output_kernel, n_tp, len(edges)),
        tuple(like((rows, columns), f32 if k == 0 else bf16) for k in range(n_tp)),
        (
            jnp.stack([place_tp ^ k for k in range(n_tp)]).astype(jnp.int32),
            masks,
            own1,
            got1,
            own2,
            got2,
            *edges,
            conv_kernel,
            y_attn,
            w_out_conv,
            w_out_attn,
        ),
        scalars=2,
        name="output",
        flops=4 * rows * width * features,
    )
    result = shares[0]
    for k in range(n_tp - 1, 0, -1):
        result = result + swap(shares[k], "tp", k).astype(f32)
    return result.astype(bf16)


def solution(mesh):
    placed = (
        P(("grp", "sp"), "tp"),
        P(),
        P("sp", "tp"),
        P("sp", "tp"),
        P("sp", "tp"),
        P(None, "tp"),
        P(None, "tp"),
        P(None, "tp"),
        P(),
        P(),
        P(),
        P(None, "tp"),
        P(None, "tp"),
        P(None, "tp"),
        P(None, "tp"),
        P("tp", None),
        P("tp", None),
    )
    sp, tp = mesh.shape["sp"], mesh.shape["tp"]
    few = all(2 <= n <= DIRECT and n & (n - 1) == 0 for n in (sp, tp))
    return jax.shard_map(
        per_device if few else per_device_wide, mesh=mesh, in_specs=placed, out_specs=P(("grp", "sp"), "tp"), check_vma=False
    )
```
